32 devices in a mesh: sp: 8 (over z, y), tp: 4 (over x, core).
Axes of the slice: x: 2, y: 2, z: 4, core: 2. Of those that a mesh axis runs over, the one named last changes fastest.
Arguments:
- stream: bfloat16 [3072, 2048], P(('sp', 'tp')), may hold values from -6 to 6
- query_projected: bfloat16 [3072, 1024], P('sp', 'tp'), may hold values from -6 to 6
- key_projected: bfloat16 [3072, 1024], P('sp', 'tp'), may hold values from -6 to 6
- value_projected: bfloat16 [3072, 1024], P('sp', 'tp'), may hold values from -6 to 6
- gate_projected: bfloat16 [3072, 1024], P('sp', 'tp'), may hold values from -6 to 6
- strength_logits: bfloat16 [8, 3072], P('tp', 'sp'), may hold values from -7 to 4
- decay_preactivation: bfloat16 [8, 3072], P('tp', 'sp'), may hold values from -9 to 9
- extra_log_decay: float32 [8, 3072], P('tp', 'sp'), may hold values from -0.7 to 0
- head_decay_rate: float32 [8], P('tp'), may hold values from 0 to 0.1
- head_norm_gain: float32 [128], replicated, may hold values from 0.1 to 1.9
- head_output_matrix: bfloat16 [1024, 2048], P('tp'), may hold values from -0.1875 to 0.1875
- feed_norm_gain: float32 [2048], replicated, may hold values from 0.1 to 1.9
- gate_matrix: bfloat16 [2048, 5632], P('sp', 'tp'), may hold values from -0.125 to 0.125
- up_matrix: bfloat16 [2048, 5632], P('sp', 'tp'), may hold values from -0.125 to 0.125
- down_matrix: bfloat16 [5632, 2048], P('tp', 'sp'), may hold values from -0.078125 to 0.078125
Outputs:
- result: bfloat16 [3072, 2048], P(('sp', 'tp'))
The draws below stay inside these ranges and needn't reach their ends.
All inputs are finite; a program needn't handle non-finite values.
Results may differ from the reference program's by a relative error of at most 0.015.
Values may be sent and summed in bfloat16 or wider, within the bound.
A program may use at most 128 MiB of HBM per device.

```python
import math
import jax
import jax.numpy as jnp
from jax import lax

D = 2048
HEADS = 8
HEAD = 128
FF = 5632
BLOCK = 64
TOK_DEV = 384
HK = 1024
TOKENS = 3072
N_TP = 4


def head_ranking(key):
    return jax.random.permutation(jax.random.fold_in(key, 101), HEADS)


def fast_heads(key):
    fast_count = HEADS // 2
    return head_ranking(key) < fast_count


def draw_head_decay_rate(key, part):
    is_fast = fast_heads(key)
    slow_rate = jnp.exp(jax.random.uniform(jax.random.fold_in(key, 102), (HEADS,), jnp.float32, math.log(0.01), math.log(0.3))) / TOKENS
    fast_rate = jnp.exp(jax.random.uniform(jax.random.fold_in(key, 103), (HEADS,), jnp.float32, math.log(0.03), math.log(0.1)))
    return jnp.where(is_fast, fast_rate, slow_rate).astype(jnp.float32)


def draw_strength_logits(key, part):
    is_fast = fast_heads(key)
    fast_part = jnp.clip(jax.random.normal(jax.random.fold_in(key, 401), (HEADS, TOKENS), jnp.float32), -4.0, 4.0)
    faint_part = jax.random.uniform(jax.random.fold_in(key, 402), (HEADS, TOKENS), jnp.float32, -7.0, -5.0)
    return jnp.where(is_fast[:, None], fast_part, faint_part).astype(jnp.bfloat16)


def draw_decay_preactivation(key, part):
    block_total = TOKENS // TOK_DEV
    noise = jnp.clip(jax.random.normal(jax.random.fold_in(key, 201), (HEADS, block_total, TOK_DEV), jnp.float32), -6.0, 6.0)
    offsets = jax.random.uniform(jax.random.fold_in(key, 202), (block_total,), jnp.float32, -1.5, 1.5)
    return (noise + offsets[None, :, None]).reshape(HEADS, TOKENS).astype(jnp.bfloat16)


def draw_extra_log_decay(key, part):
    places = jax.random.randint(jax.random.fold_in(key, 301), (3,), 0, TOKENS)
    levels = jax.random.uniform(jax.random.fold_in(key, 302), (HEADS, 3), jnp.float32, math.log(0.5), math.log(0.8))
    base = jnp.zeros((HEADS, TOKENS), jnp.float32)
    return base.at[:, places].set(levels).astype(jnp.float32)


def steps_of(stream_key, extent, pieces, low, largest):
    def one(dim, blocks):
        heights = jax.random.uniform(jax.random.fold_in(jax.random.fold_in(stream_key, 6), dim), (blocks,), jnp.float32, low / len(pieces), largest / len(pieces))
        return jnp.repeat(jnp.exp(heights), extent[dim] // blocks).reshape((-1,) + (1,) * (len(extent) - dim - 1))

    level = one(*pieces[0])
    for cut in pieces[1:]:
        level = level * one(*cut)
    return level


def bell_draw(own_key, extent, scale, reach, cuts=(), kind=jnp.bfloat16):
    loudness = steps_of(own_key, extent, cuts, -0.22, 0.18) if cuts else 1.0
    values = jax.random.normal(own_key, extent, jnp.float32) * scale * loudness
    return jnp.minimum(jnp.maximum(values, -reach), reach).astype(kind)


def setup_inputs(seed: int = 0) -> dict:
    seeds = jax.random.split(jax.random.key(seed), 16)
    stream = bell_draw(seeds[0], (TOKENS, D), 1.0, 6.0, ((0, 32),))
    query_projected = bell_draw(seeds[1], (TOKENS, HK), 1.0, 6.0, ((0, 8), (1, 4)))
    key_projected = bell_draw(seeds[2], (TOKENS, HK), 1.0, 6.0, ((0, 8), (1, 4)))
    value_projected = bell_draw(seeds[3], (TOKENS, HK), 1.0, 6.0, ((0, 8), (1, 4)))
    gate_projected = bell_draw(seeds[4], (TOKENS, HK), 1.0, 6.0, ((0, 8), (1, 4)))
    strength_logits = draw_strength_logits(jax.random.fold_in(seeds[15], 71), 0)
    decay_preactivation = draw_decay_preactivation(jax.random.fold_in(seeds[15], 71), 0)
    extra_log_decay = draw_extra_log_decay(jax.random.fold_in(seeds[15], 71), 0)
    head_decay_rate = draw_head_decay_rate(jax.random.fold_in(seeds[15], 71), 0)
    head_norm_gain = jnp.clip(1.0 + 0.18 * jax.random.normal(seeds[9], (HEAD,), jnp.float32), 0.1, 1.9)
    head_output_matrix = bell_draw(seeds[10], (HK, D), HK ** -0.5, 0.1875, ((0, 4),))
    feed_norm_gain = jnp.clip(1.0 + 0.18 * jax.random.normal(seeds[11], (D,), jnp.float32), 0.1, 1.9)
    gate_matrix = bell_draw(seeds[12], (D, FF), D ** -0.5, 0.125, ((0, 8), (1, 4)))
    up_matrix = bell_draw(seeds[13], (D, FF), D ** -0.5, 0.125, ((0, 8), (1, 4)))
    down_matrix = bell_draw(seeds[14], (FF, D), FF ** -0.5, 0.078125, ((0, 4), (1, 8)))
    return dict(stream=stream, query_projected=query_projected, key_projected=key_projected, value_projected=value_projected, gate_projected=gate_projected, strength_logits=strength_logits, decay_preactivation=decay_preactivation, extra_log_decay=extra_log_decay, head_decay_rate=head_decay_rate, head_norm_gain=head_norm_gain, head_output_matrix=head_output_matrix, feed_norm_gain=feed_norm_gain, gate_matrix=gate_matrix, up_matrix=up_matrix, down_matrix=down_matrix)


PRECISION_FULL = lax.Precision.HIGHEST
EPSILON = 1e-06

def unit_rows(tensor):
    return tensor * lax.rsqrt(lax.optimization_barrier(jnp.sum(tensor * tensor, axis=-1, keepdims=True)) + EPSILON)

def block_correction(unit_queries, unit_keys, complete_values, strength_logits, decay_preactivation, extra_log_decay, head_decay_rate):
    head_count, length, head_width = unit_queries.shape
    block_count = length // BLOCK

    def to_blocks(tensor):
        return tensor.reshape((head_count, block_count, BLOCK) + tensor.shape[2:])
    beta_gate = jax.nn.sigmoid(strength_logits.astype(jnp.float32))
    decay_logarithm = -head_decay_rate[:, None] * jax.nn.softplus(decay_preactivation.astype(jnp.float32)) + extra_log_decay
    query_block = to_blocks(unit_queries)
    key_block = to_blocks(unit_keys)
    value_block = to_blocks(complete_values)
    beta_block = to_blocks(beta_gate)
    cumulative = jnp.cumsum(to_blocks(decay_logarithm), axis=-1)
    causal = jnp.tril(jnp.ones((BLOCK, BLOCK), bool))
    strict = jnp.tril(jnp.ones((BLOCK, BLOCK), bool), -1)
    spread = cumulative[..., :, None] - cumulative[..., None, :]
    damping = jnp.where(causal, jnp.exp(jnp.where(causal, spread, 0.0)), 0.0)
    key_beta = key_block * beta_block[..., None]
    lower_part = jnp.einsum('hnid,hnjd->hnij', key_beta, key_block, precision=PRECISION_FULL) * jnp.where(strict, damping, 0.0)
    system = lower_part + jnp.eye(BLOCK, dtype=jnp.float32)
    right_side = jnp.concatenate([value_block * beta_block[..., None], key_beta * jnp.exp(cumulative)[..., None]], axis=-1)
    solved = lax.linalg.triangular_solve(system, right_side, left_side=True, lower=True, unit_diagonal=True)
    target_values = solved[..., :head_width]
    householder_weights = solved[..., head_width:]
    inner_scores = jnp.einsum('hnid,hnjd->hnij', query_block, key_block, precision=PRECISION_FULL) * damping
    decayed_queries = query_block * jnp.exp(cumulative)[..., None]
    closing_log_decay = cumulative[..., -1:]
    decayed_keys = key_block * jnp.exp(closing_log_decay - cumulative)[..., None]
    return (decayed_queries, decayed_keys, target_values, householder_weights, inner_scores, closing_log_decay)

def advance(running_state, items):
    decayed_queries, decayed_keys, target_values, householder_weights, inner_scores, closing_log_decay = items
    new_state = target_values - jnp.einsum('fdc,fcj->fdj', householder_weights, running_state, precision=PRECISION_FULL)
    layer_output = jnp.einsum('fdc,fcj->fdj', decayed_queries, running_state, precision=PRECISION_FULL)
    layer_output = layer_output + jnp.einsum('hij,hjv->hiv', inner_scores, new_state, precision=PRECISION_FULL)
    running_state = jnp.exp(closing_log_decay)[:, :, None] * running_state + jnp.einsum('xwp,xws->xps', decayed_keys, new_state, precision=PRECISION_FULL)
    return (running_state, layer_output)

def split_heads(tensor):
    return tensor.reshape(TOKENS, HEADS, HEAD).transpose(1, 0, 2).astype(jnp.float32)

def rms_scale(tensor):
    return tensor * lax.rsqrt(lax.optimization_barrier(jnp.mean(tensor * tensor, axis=-1, keepdims=True)) + EPSILON)

def reference(stream, query_projected, key_projected, value_projected, gate_projected, strength_logits, decay_preactivation, extra_log_decay, head_decay_rate, head_norm_gain, head_output_matrix, feed_norm_gain, gate_matrix, up_matrix, down_matrix):
    unit_queries = unit_rows(split_heads(query_projected)) * HEAD ** (-0.5)
    unit_keys = unit_rows(split_heads(key_projected))
    complete_values = split_heads(value_projected)
    score_terms = block_correction(unit_queries, unit_keys, complete_values, strength_logits, decay_preactivation, extra_log_decay, head_decay_rate)
    moved = tuple((jnp.moveaxis(tensor, 1, 0) for tensor in score_terms))
    initial = jnp.zeros((HEADS, HEAD, HEAD), jnp.float32)
    _, block_outputs = lax.scan(advance, initial, moved)
    attention_output = jnp.moveaxis(block_outputs, 0, 1).reshape(HEADS, TOKENS, HEAD)
    normed_heads = rms_scale(attention_output) * head_norm_gain
    gated = normed_heads.transpose(1, 0, 2).reshape(TOKENS, HK) * jax.nn.silu(gate_projected.astype(jnp.float32))
    mixed = gated.astype(jnp.bfloat16)
    group_width = HK // N_TP
    branch = jnp.zeros((TOKENS, D), jnp.float32)
    for group in range(N_TP):
        piece = jnp.dot(mixed[:, group * group_width:(group + 1) * group_width].astype(jnp.float32), head_output_matrix[group * group_width:(group + 1) * group_width].astype(jnp.float32), preferred_element_type=jnp.float32)
        branch = branch + piece.astype(jnp.bfloat16).astype(jnp.float32)
    residual = stream.astype(jnp.float32) + branch
    normed = (rms_scale(residual) * feed_norm_gain).astype(jnp.bfloat16)
    gate = jnp.dot(normed.astype(jnp.float32), gate_matrix.astype(jnp.float32), preferred_element_type=jnp.float32)
    up_value = jnp.dot(normed.astype(jnp.float32), up_matrix.astype(jnp.float32), preferred_element_type=jnp.float32)
    hidden = (jax.nn.silu(gate) * up_value).astype(jnp.bfloat16)
    unit_group = FF // N_TP
    ffn_total = jnp.zeros((TOKENS, D), jnp.float32)
    for group in range(N_TP):
        piece = jnp.dot(hidden[:, group * unit_group:(group + 1) * unit_group].astype(jnp.float32), down_matrix[group * unit_group:(group + 1) * unit_group].astype(jnp.float32), preferred_element_type=jnp.float32)
        ffn_total = ffn_total + piece.astype(jnp.bfloat16).astype(jnp.float32)
    return (residual + ffn_total).astype(jnp.bfloat16)
```

```python
import functools

import jax
import jax.numpy as jnp
from jax import lax
from jax.experimental import pallas as pl
from jax.experimental.pallas import tpu as pltpu
from jax.sharding import PartitionSpec as P

HEAD = 128
CHUNK = 128
EPSILON = 1e-06
F32 = jnp.float32
BF16 = jnp.bfloat16
HIGHEST = lax.Precision.HIGHEST
NN = (((1,), (0,)), ((), ()))
NT = (((1,), (1,)), ((), ()))
TN = (((0,), (0,)), ((), ()))


def dot1(a, b, dims=NN):
    return lax.dot_general(a, b, dims, preferred_element_type=F32)


def halves(x):
    high = x.astype(BF16)
    return high, (x - high.astype(F32)).astype(BF16)


def dot3(a, b, dims=NN):
    ah, al = halves(a)
    bh, bl = halves(b)
    return dot1(ah, bh, dims) + (dot1(ah, bl, dims) + dot1(al, bh, dims))


def silu(x):
    return x * jax.nn.sigmoid(x)


def messages(ring):
    half = ring // 2
    first, relay_gate, relay_up, relay_down, late = [], [], [], [], []
    for a in "GU":
        for way in "RLY":
            first.append((a, 0, 0, way))
    for k in range(2, half + 1):
        relay_gate.append(("G", -(k - 1), 0, "R"))
        if k < half:
            relay_gate.append(("G", k - 1, 0, "L"))
    for k in range(1, half):
        relay_gate.append(("G", -k, 0, "Y"))
        relay_gate.append(("G", k, 0, "Y"))
    far_gate = [("G", half, 0, "Y")] if half else []
    for k in range(1, half + 1):
        for rel in (1, 0):
            if (k > 1 or rel == 1) and (k < half or rel == 0):
                relay_up.append(("U", -(k - 1), rel, "R"))
            if (k > 1 or rel == 1) and (k < half or rel == 1):
                relay_up.append(("U", k - 1, rel, "L"))
    down_own = [("D", 0, 0, way) for way in "RLY"]
    for k in range(1, half + 1):
        for rel in (1, 0):
            if (k > 1 or rel == 1) and k < half:
                relay_down.append(("D", -(k - 1), rel, "R"))
            if (k > 1 or rel == 1) and (k < half or rel == 0):
                relay_down.append(("D", k - 1, rel, "L"))
    late.append(("D", half, 0, "Y"))
    return first, relay_gate, far_gate, relay_up, down_own, relay_down, late


def kernel(
    n, tps, groups,
    stream, qp, kp, vp, gp, strength, decay_pre, extra, rate, head_gain, w_out, feed_gain,
    gate_in, up_in, down_in,
    result,
    gate_all, up_all, down_all, out_scr, x_send, x_part, p_send, p_recv, s_in, mixed,
    d_send, d_recv, residual, rows_all, hidden, f_part, f_recv,
    w_send, w_recv, own_sem, x_sem, p_ssem, p_rsem, d_ssem, d_rsem, e_ssem, e_rsem, f_ssem, f_rsem,
):
    ring = n // 2
    sp = lax.axis_index("sp")
    tp = lax.axis_index("tp")
    r = sp // 2
    p = lax.rem(sp, 2)
    heads = strength.shape[0]
    tokens = strength.shape[1]
    chunks = tokens // CHUNK
    own_rows = stream.shape[0]
    kr = gate_in.shape[0]
    MESH = pl.DeviceIdType.MESH

    def sp_of(dr, rel):
        q = p if rel == 0 else 1 - p
        return lax.rem(r + dr + ring, ring) * 2 + q

    partner = sp_of(0, 1)
    where = {"R": sp_of(1, 0), "L": sp_of(-1, 0), "Y": partner}

    def tp_peer(o):
        return lax.rem(tp + o, tps)

    barrier = pltpu.get_barrier_semaphore()
    for dr in range(1, ring):
        pl.semaphore_signal(barrier, 1, device_id=(sp_of(dr, 0), tp), device_id_type=MESH)
    pl.semaphore_signal(barrier, 1, device_id=(partner, tp), device_id_type=MESH)
    for o in range(1, tps):
        pl.semaphore_signal(barrier, 1, device_id=(sp, tp_peer(o)), device_id_type=MESH)
    pl.semaphore_wait(barrier, ring + tps - 1)

    flat = [m for g in groups for m in g]
    number = {m: i for i, m in enumerate(flat)}
    arrival = {}
    for (a, dr, rel, way) in flat:
        to = {"R": (dr - 1, rel), "L": (dr + 1, rel), "Y": (dr, 1 - rel)}[way]
        key = (a, to[0] % ring, to[1])
        assert key not in arrival
        arrival[key] = number[(a, dr, rel, way)]
    waited = set()
    copies = []

    def slot(a, dr, rel):
        s = sp_of(dr, rel)
        if a == "D":
            return down_all.at[s]
        whole = gate_all if a == "G" else up_all
        return whole.at[pl.ds(pl.multiple_of(s * kr, kr), kr), :]

    inputs = {"G": gate_in, "U": up_in, "D": down_in}

    def need(a, dr, rel):
        dr = dr % ring
        key = (a, dr, rel)
        if (dr == 0 and rel == 0) or key in waited:
            return
        waited.add(key)
        m = arrival[key]
        here = slot(*key)
        pltpu.make_async_remote_copy(
            here, here, w_send.at[m], w_recv.at[m], device_id=(partner, tp), device_id_type=MESH
        ).wait_recv()

    def pump(group):
        for message in group:
            a, dr, rel, way = message
            need(a, dr, rel)
            own = dr % ring == 0 and rel == 0
            m = number[message]
            copy = pltpu.make_async_remote_copy(
                inputs[a] if own else slot(a, dr % ring, rel),
                slot(a, dr % ring, rel),
                w_send.at[m], w_recv.at[m],
                device_id=(where[way], tp), device_id_type=MESH,
            )
            copy.start()
            copies.append(copy)

    first, relay_gate, far_gate, relay_up, down_own, relay_down, late = groups
    pump(first)
    locals_ = []
    for i, a in enumerate("GUD"):
        local = pltpu.make_async_copy(inputs[a], slot(a, 0, 0), own_sem.at[i])
        local.start()
        locals_.append(local)

    row_i = lax.broadcasted_iota(jnp.int32, (CHUNK, CHUNK), 0)
    col_i = lax.broadcasted_iota(jnp.int32, (CHUNK, CHUNK), 1)
    causal = row_i >= col_i
    strict = row_i > col_i
    eye = jnp.where(row_i == col_i, 1.0, 0.0).astype(F32)
    lower = jnp.where(causal, 1.0, 0.0).astype(F32)
    beta = jax.nn.sigmoid(strength[...].astype(F32))
    pre = decay_pre[...].astype(F32)
    soft = jnp.maximum(pre, 0.0) + jnp.log1p(jnp.exp(-jnp.abs(pre)))
    log_decay = -rate[...] * soft + extra[...]

    pairs = [(h, c) for c in range(chunks) for h in range(heads)]
    data = {}
    for c in range(chunks):
        span = slice(c * CHUNK, (c + 1) * CHUNK)
        ld = log_decay[:, span]
        c_row = lax.dot_general(ld, lower, NT, precision=HIGHEST, preferred_element_type=F32)
        c_col = lax.dot_general(lower, ld, NT, precision=HIGHEST, preferred_element_type=F32)
        b_col = lax.dot_general(eye, beta[:, span], NT, precision=HIGHEST, preferred_element_type=F32)
        for h in range(heads):
            lanes = slice(h * HEAD, (h + 1) * HEAD)
            q = qp[span, lanes].astype(F32)
            k = kp[span, lanes].astype(F32)
            v = vp[span, lanes].astype(F32)
            q = q * (lax.rsqrt(jnp.sum(q * q, axis=-1, keepdims=True) + EPSILON) * HEAD ** (-0.5))
            k = k * lax.rsqrt(jnp.sum(k * k, axis=-1, keepdims=True) + EPSILON)
            cc = c_col[:, h:h + 1]
            bb = b_col[:, h:h + 1]
            cr = c_row[h:h + 1, :]
            last = cr[:, CHUNK - 1:]
            damp = jnp.where(causal, jnp.exp(jnp.where(causal, cc - cr, 0.0)), 0.0)
            grown = jnp.exp(cc)
            kb = k * bb
            kk = dot3(kb, k, NT) * jnp.where(strict, damp, 0.0)
            inner = dot3(q, k, NT) * damp
            data[h, c] = dict(
                low=kk, inner=inner, v=v * bb, kw=kb * grown, qd=q * grown,
                kd=k * jnp.exp(last - cc), decay=jnp.exp(last),
            )
    inverse = {}
    b = 1
    shift = 0
    while b < CHUNK:
        mask = ((row_i >> (shift + 1)) == (col_i >> (shift + 1))) & (
            ((row_i >> shift) & 1) == 1) & (((col_i >> shift) & 1) == 0)
        for key in pairs:
            piece = jnp.where(mask, data[key]["low"], 0.0)
            if b == 1:
                inverse[key] = eye - piece
            else:
                x = inverse[key]
                inverse[key] = x - dot3(x, dot3(piece, x))
        b *= 2
        shift += 1
    states = [jnp.concatenate([jnp.zeros((HEAD, HEAD), F32), eye], axis=1) for _ in range(heads)]
    for c in range(chunks):
        for h in range(heads):
            e = data[h, c]
            u = dot3(inverse[h, c], e["v"])
            w = dot3(inverse[h, c], e["kw"])
            x = states[h]
            new = jnp.concatenate([u, jnp.zeros_like(u)], axis=1) - dot3(w, x)
            out_scr[h, c * CHUNK:(c + 1) * CHUNK, :] = dot3(e["qd"], x) + dot3(e["inner"], new)
            states[h] = e["decay"] * x + dot3(e["kd"], new, TN)

    for h in range(heads):
        x_send[h] = states[h].astype(BF16)
    x_copy = pltpu.make_async_remote_copy(
        x_send, x_part, x_sem.at[0], x_sem.at[1], device_id=(partner, tp), device_id_type=MESH)
    x_copy.start()
    x_copy.wait_recv()
    for h in range(heads):
        mine = states[h]
        theirs = x_part[h].astype(F32)
        before = jnp.where(p == 0, mine, theirs)
        after = jnp.where(p == 0, theirs, mine)
        after_s = jnp.concatenate([after[:, :HEAD], jnp.zeros((HEAD, HEAD), F32)], axis=1)
        p_send[h] = (dot3(after[:, HEAD:], before) + after_s).astype(BF16)

    def p_copy(k, to, at):
        return pltpu.make_async_remote_copy(
            p_send, p_recv.at[at], p_ssem.at[k], p_rsem.at[k],
            device_id=(to, tp), device_id_type=MESH)

    for k in range(1, ring):
        @pl.when(r + k < ring)
        def _():
            p_copy(k, sp_of(k, 0), r).start()
    pump(relay_gate)
    for k in range(1, ring):
        @pl.when(r - k >= 0)
        def _():
            p_copy(k, sp_of(-k, 0), r - k).wait_recv()
    s_in[...] = jnp.zeros_like(s_in)

    def fold(i, _):
        for h in range(heads):
            got = p_recv[i, h].astype(F32)
            s_in[h] = dot3(got[:, HEAD:], s_in[h]) + got[:, :HEAD]
        return 0

    lax.fori_loop(0, r, fold, 0)
    for h in range(heads):
        lanes = slice(h * HEAD, (h + 1) * HEAD)
        got = x_part[h].astype(F32)
        s = s_in[h]
        s = jnp.where(p == 0, s, dot3(got[:, HEAD:], s) + got[:, :HEAD])
        att = out_scr[h, :, :HEAD] + dot3(out_scr[h, :, HEAD:], s)
        att = att * lax.rsqrt(jnp.mean(att * att, axis=-1, keepdims=True) + EPSILON) * head_gain[...]
        mixed[:, lanes] = (att * silu(gp[:, lanes].astype(F32))).astype(BF16)

    def rows_of(t):
        return pl.ds(pl.multiple_of(t * own_rows, own_rows), own_rows)

    order = [o for o in (2, 3, 1) if o < tps] + list(range(4, tps))
    d_copies = []
    for o in order:
        to = tp_peer(o)
        d_send[o - 1] = dot1(mixed[rows_of(to), :], w_out[...]).astype(BF16)
        copy = pltpu.make_async_remote_copy(
            d_send.at[o - 1], d_recv.at[o - 1], d_ssem.at[o - 1], d_rsem.at[o - 1],
            device_id=(sp, to), device_id_type=MESH)
        copy.start()
        d_copies.append(copy)
    pump(relay_up)
    pump(far_gate)
    total = dot1(mixed[rows_of(tp), :], w_out[...]).astype(BF16).astype(F32)
    for copy in d_copies:
        copy.wait_recv()
    for o in range(1, tps):
        total = total + d_recv[o - 1].astype(F32)
    total = stream[...].astype(F32) + total
    residual[...] = total
    rows_all[rows_of(tp), :] = (
        total * lax.rsqrt(jnp.mean(total * total, axis=-1, keepdims=True) + EPSILON) * feed_gain[...]
    ).astype(BF16)
    e_copies = []
    for o in order:
        copy = pltpu.make_async_remote_copy(
            rows_all.at[rows_of(tp), :], rows_all.at[rows_of(tp), :], e_ssem.at[o - 1], e_rsem.at[o - 1],
            device_id=(sp, tp_peer(o)), device_id_type=MESH)
        copy.start()
        e_copies.append(copy)
    pump(down_own)
    for o in order:
        there = rows_all.at[rows_of(lax.rem(tp - o + tps, tps)), :]
        pltpu.make_async_remote_copy(
            there, there, e_ssem.at[o - 1], e_rsem.at[o - 1],
            device_id=(sp, tp_peer(o)), device_id_type=MESH).wait_recv()
    for a in "GU":
        for dr in range(ring):
            for rel in (0, 1):
                need(a, dr, rel)
    for local in locals_:
        local.wait()
    pump(relay_down)

    tile = 128

    def ffn_in(i, _):
        lanes = pl.ds(pl.multiple_of(i * tile, tile), tile)
        both = dot1(rows_all[...], jnp.concatenate([gate_all[:, lanes], up_all[:, lanes]], axis=1))
        hidden[:, lanes] = (silu(both[:, :tile]) * both[:, tile:]).astype(BF16)
        return 0

    lax.fori_loop(0, gate_all.shape[1] // tile, ffn_in, 0)
    pump(late)
    for dr in range(ring):
        for rel in (0, 1):
            need("D", dr, rel)
    dc = down_all.shape[2]
    pack = max(1, 128 // dc)
    wide = pack * dc

    def ffn_out(i, _):
        lanes = pl.ds(pl.multiple_of(i * wide, wide), wide)
        if pack == 1:
            weights = down_all[i]
        else:
            weights = jnp.concatenate([down_all[i * pack + j] for j in range(pack)], axis=1)
        f_part[:, lanes] = dot1(hidden[...], weights).astype(BF16)
        return 0

    lax.fori_loop(0, n // pack, ffn_out, 0)
    f_copies = []
    for o in order:
        copy = pltpu.make_async_remote_copy(
            f_part.at[rows_of(tp_peer(o)), :], f_recv.at[o - 1], f_ssem.at[o - 1], f_rsem.at[o - 1],
            device_id=(sp, tp_peer(o)), device_id_type=MESH)
        copy.start()
        f_copies.append(copy)
    ffn = f_part[rows_of(tp), :].astype(F32)
    for copy in f_copies:
        copy.wait_recv()
    for o in range(1, tps):
        ffn = ffn + f_recv[o - 1].astype(F32)
    result[...] = (residual[...] + ffn).astype(BF16)

    for copy in copies + [x_copy] + d_copies + e_copies + f_copies:
        copy.wait_send()
    for k in range(1, ring):
        @pl.when(r + k < ring)
        def _():
            p_copy(k, sp_of(k, 0), r).wait_send()


def body(n, tps, stream, qp, kp, vp, gp, strength, decay_pre, extra, rate, head_gain, w_out,
         feed_gain, gate_m, up_m, down_m):
    heads, tokens = strength.shape
    own, width = stream.shape
    kr, units = gate_m.shape
    ring = n // 2
    groups = messages(ring)
    count = sum(len(g) for g in groups)
    dma = pltpu.SemaphoreType.DMA
    vmem = pl.BlockSpec(memory_space=pltpu.VMEM)
    hbm = pl.BlockSpec(memory_space=pl.ANY)
    peers = max(1, tps - 1)
    return pl.pallas_call(
        functools.partial(kernel, n, tps, groups),
        out_shape=jax.ShapeDtypeStruct((own, width), BF16),
        in_specs=[vmem] * 12 + [hbm] * 3,
        out_specs=vmem,
        scratch_shapes=[
            pltpu.VMEM((kr * n, units), BF16),
            pltpu.VMEM((kr * n, units), BF16),
            pltpu.VMEM((n,) + down_m.shape, BF16),
            pltpu.VMEM((heads, tokens, 2 * HEAD), F32),
            pltpu.VMEM((heads, HEAD, 2 * HEAD), BF16),
            pltpu.VMEM((heads, HEAD, 2 * HEAD), BF16),
            pltpu.VMEM((heads, HEAD, 2 * HEAD), BF16),
            pltpu.VMEM((ring, heads, HEAD, 2 * HEAD), BF16),
            pltpu.VMEM((heads, HEAD, HEAD), F32),
            pltpu.VMEM((tokens, heads * HEAD), BF16),
            pltpu.VMEM((peers, own, width), BF16),
            pltpu.VMEM((peers, own, width), BF16),
            pltpu.VMEM((own, width), F32),
            pltpu.VMEM((tokens, width), BF16),
            pltpu.VMEM((tokens, units), BF16),
            pltpu.VMEM((tokens, width), BF16),
            pltpu.VMEM((peers, own, width), BF16),
            dma((count,)), dma((count,)), dma((3,)), dma((2,)), dma((ring,)), dma((ring,)),
            dma((peers,)), dma((peers,)), dma((peers,)), dma((peers,)), dma((peers,)), dma((peers,)),
        ],
        compiler_params=pltpu.CompilerParams(
            collective_id=0, has_side_effects=True, vmem_limit_bytes=60 * 1024 * 1024),
    )(stream, qp, kp, vp, gp, strength, decay_pre, extra, rate[:, None], head_gain[None, :], w_out,
      feed_gain[None, :], gate_m, up_m, down_m)


def solution(mesh):
    placed = (
        P(("sp", "tp"), None),
        P("sp", "tp"),
        P("sp", "tp"),
        P("sp", "tp"),
        P("sp", "tp"),
        P("tp", "sp"),
        P("tp", "sp"),
        P("tp", "sp"),
        P("tp"),
        P(),
        P("tp", None),
        P(),
        P("sp", "tp"),
        P("sp", "tp"),
        P("tp", "sp"),
    )
    return jax.shard_map(
        functools.partial(body, mesh.shape["sp"], mesh.shape["tp"]),
        mesh=mesh, in_specs=placed, out_specs=P(("sp", "tp"), None), check_vma=False,
    )
```

```python
import functools

import jax
import jax.numpy as jnp
from jax import lax
from jax.experimental import pallas as pl
from jax.experimental.pallas import tpu as pltpu
from jax.sharding import PartitionSpec as P

HEAD = 128
CHUNK = 128
EPSILON = 1e-06
F32 = jnp.float32
BF16 = jnp.bfloat16
HIGHEST = lax.Precision.HIGHEST
NN = (((1,), (0,)), ((), ()))
NT = (((1,), (1,)), ((), ()))
TN = (((0,), (0,)), ((), ()))


def dot1(a, b, dims=NN):
    return lax.dot_general(a, b, dims, preferred_element_type=F32)


def halves(x):
    high = x.astype(BF16)
    return high, (x - high.astype(F32)).astype(BF16)


def dot3(a, b, dims=NN):
    ah, al = halves(a)
    bh, bl = halves(b)
    return dot1(ah, bh, dims) + (dot1(ah, bl, dims) + dot1(al, bh, dims))


def silu(x):
    return x * jax.nn.sigmoid(x)


def messages(ring):
    own_z = [(a, 0, 0, way) for a in "GU" for way in "RL"]
    own_y = [(a, 0, 0, "Y") for a in "GU"]
    first = own_z + own_y
    down_y = [("D", 0, 0, "Y")]

    def relay(a, j, skip_y=False):
        out = []
        if j < ring - 1:
            out += [(a, -j, 0, "R"), (a, j, 0, "L")]
        if not skip_y:
            out += [(a, -j, 0, "Y"), (a, j, 0, "Y")]
        return out

    early, middle, later, last = [], [], [], []
    if ring > 1:
        early = relay("G", 1)
        middle = relay("U", 1)
        for j in range(2, ring):
            later += relay("G", j) + relay("U", j)
            if j == 2:
                later += [("D", 0, 0, "R"), ("D", 0, 0, "L")]
        if ring == 2:
            later += [("D", 0, 0, "R"), ("D", 0, 0, "L")]
        later += [("D", 0, 1, "R"), ("D", 0, 1, "L")]
        later += relay("D", 1, skip_y=True)
        for j in range(2, ring):
            last += relay("D", j)
    else:
        first = own_y
    return first, down_y, early, middle, later, last


def kernel(
    n, tps, groups,
    stream, qp, kp, vp, gp, strength, decay_pre, extra, rate, head_gain, w_out, feed_gain,
    gate_in, up_in, down_in,
    result,
    gate_all, up_all, down_all, out_scr, x_send, x_part, p_send, p_recv, s_in, mixed,
    d_send, d_recv, residual, rows_all, hidden, f_part, f_recv,
    w_send, w_recv, own_sem, x_sem, p_ssem, p_rsem, d_ssem, d_rsem, e_ssem, e_rsem, f_ssem, f_rsem,
):
    ring = n // 2
    sp = lax.axis_index("sp")
    tp = lax.axis_index("tp")
    r = sp // 2
    p = lax.rem(sp, 2)
    heads = strength.shape[0]
    tokens = strength.shape[1]
    chunks = tokens // CHUNK
    own_rows = stream.shape[0]
    kr = gate_in.shape[0]
    MESH = pl.DeviceIdType.MESH

    def sp_of(dr, rel):
        q = p if rel == 0 else 1 - p
        return lax.rem(r + dr + ring, ring) * 2 + q

    partner = sp_of(0, 1)
    where = {"R": sp_of(1, 0), "L": sp_of(-1, 0), "Y": partner}

    def tp_peer(o):
        return lax.rem(tp + o, tps)

    barrier = pltpu.get_barrier_semaphore()
    for dr in range(1, ring):
        pl.semaphore_signal(barrier, 1, device_id=(sp_of(dr, 0), tp), device_id_type=MESH)
    pl.semaphore_signal(barrier, 1, device_id=(partner, tp), device_id_type=MESH)
    for o in range(1, tps):
        pl.semaphore_signal(barrier, 1, device_id=(sp, tp_peer(o)), device_id_type=MESH)
    pl.semaphore_wait(barrier, ring + tps - 1)

    flat = [m for g in groups for m in g]
    number = {m: i for i, m in enumerate(flat)}
    arrival = {}
    for (a, dr, rel, way) in flat:
        to = {"R": (dr - 1, rel), "L": (dr + 1, rel), "Y": (dr, 1 - rel)}[way]
        key = (a, to[0], to[1])
        assert key not in arrival
        arrival[key] = number[(a, dr, rel, way)]
    waited = set()
    copies = []

    def exists(dr):
        return (r + dr >= 0) & (r + dr < ring)

    def slot(a, dr, rel):
        s = sp_of(dr, rel)
        if a == "D":
            return down_all.at[s]
        whole = gate_all if a == "G" else up_all
        return whole.at[pl.ds(pl.multiple_of(s * kr, kr), kr), :]

    inputs = {"G": gate_in, "U": up_in, "D": down_in}

    def need(a, dr, rel):
        key = (a, dr, rel)
        if (dr == 0 and rel == 0) or key in waited:
            return
        waited.add(key)
        m = arrival[key]

        @pl.when(exists(dr))
        def _():
            here = slot(*key)
            pltpu.make_async_remote_copy(
                here, here, w_send.at[m], w_recv.at[m], device_id=(partner, tp), device_id_type=MESH
            ).wait_recv()

    def outgoing(message):
        a, dr, rel, way = message
        m = number[message]
        return pltpu.make_async_remote_copy(
            inputs[a] if dr == 0 and rel == 0 else slot(a, dr, rel),
            slot(a, dr, rel),
            w_send.at[m], w_recv.at[m],
            device_id=(where[way], tp), device_id_type=MESH,
        )

    def goes(message):
        ahead = {"R": r + 1 < ring, "L": r >= 1, "Y": r >= 0}[message[3]]
        return exists(message[1]) & ahead

    def pump(group):
        for message in group:
            need(*message[:3])

            @pl.when(goes(message))
            def _():
                outgoing(message).start()

            copies.append(message)

    def need_all(a):
        for dr in sorted(range(1 - ring, ring), key=abs):
            for rel in (0, 1):
                need(a, dr, rel)

    first, down_y, early, middle, later, last_group = groups
    pump(first)
    locals_ = []
    for i, a in enumerate("GUD"):
        local = pltpu.make_async_copy(inputs[a], slot(a, 0, 0), own_sem.at[i])
        local.start()
        locals_.append(local)

    row_i = lax.broadcasted_iota(jnp.int32, (CHUNK, CHUNK), 0)
    col_i = lax.broadcasted_iota(jnp.int32, (CHUNK, CHUNK), 1)
    causal = row_i >= col_i
    strict = row_i > col_i
    eye = jnp.where(row_i == col_i, 1.0, 0.0).astype(F32)
    lower = jnp.where(causal, 1.0, 0.0).astype(F32)
    beta = jax.nn.sigmoid(strength[...].astype(F32))
    pre = decay_pre[...].astype(F32)
    soft = jnp.maximum(pre, 0.0) + jnp.log1p(jnp.exp(-jnp.abs(pre)))
    log_decay = -rate[...] * soft + extra[...]

    pairs = [(h, c) for c in range(chunks) for h in range(heads)]
    data = {}
    for c in range(chunks):
        span = slice(c * CHUNK, (c + 1) * CHUNK)
        ld = log_decay[:, span]
        c_row = lax.dot_general(ld, lower, NT, precision=HIGHEST, preferred_element_type=F32)
        c_col = lax.dot_general(lower, ld, NT, precision=HIGHEST, preferred_element_type=F32)
        b_col = lax.dot_general(eye, beta[:, span], NT, precision=HIGHEST, preferred_element_type=F32)
        for h in range(heads):
            lanes = slice(h * HEAD, (h + 1) * HEAD)
            q = qp[span, lanes].astype(F32)
            k = kp[span, lanes].astype(F32)
            v = vp[span, lanes].astype(F32)
            q = q * (lax.rsqrt(jnp.sum(q * q, axis=-1, keepdims=True) + EPSILON) * HEAD ** (-0.5))
            k = k * lax.rsqrt(jnp.sum(k * k, axis=-1, keepdims=True) + EPSILON)
            cc = c_col[:, h:h + 1]
            bb = b_col[:, h:h + 1]
            cr = c_row[h:h + 1, :]
            last = cr[:, CHUNK - 1:]
            damp = jnp.where(causal, jnp.exp(jnp.where(causal, cc - cr, 0.0)), 0.0)
            grown = jnp.exp(cc)
            kb = k * bb
            kk = dot3(kb, k, NT) * jnp.where(strict, damp, 0.0)
            inner = dot3(q, k, NT) * damp
            data[h, c] = dict(
                low=kk, inner=inner, v=v * bb, kw=kb * grown, qd=q * grown,
                kd=k * jnp.exp(last - cc), decay=jnp.exp(last),
            )
    inverse = {}
    b = 1
    shift = 0
    while b < CHUNK:
        mask = ((row_i >> (shift + 1)) == (col_i >> (shift + 1))) & (
            ((row_i >> shift) & 1) == 1) & (((col_i >> shift) & 1) == 0)
        for key in pairs:
            piece = jnp.where(mask, data[key]["low"], 0.0)
            if b == 1:
                inverse[key] = eye - piece
            else:
                x = inverse[key]
                inverse[key] = x - dot3(x, dot3(piece, x))
        b *= 2
        shift += 1
    states = [jnp.concatenate([jnp.zeros((HEAD, HEAD), F32), eye], axis=1) for _ in range(heads)]
    for c in range(chunks):
        for h in range(heads):
            e = data[h, c]
            u = dot3(inverse[h, c], e["v"])
            w = dot3(inverse[h, c], e["kw"])
            x = states[h]
            new = jnp.concatenate([u, jnp.zeros_like(u)], axis=1) - dot3(w, x)
            out_scr[h, c * CHUNK:(c + 1) * CHUNK, :] = dot3(e["qd"], x) + dot3(e["inner"], new)
            states[h] = e["decay"] * x + dot3(e["kd"], new, TN)

    for h in range(heads):
        x_send[h] = states[h].astype(BF16)
    x_copy = pltpu.make_async_remote_copy(
        x_send, x_part, x_sem.at[0], x_sem.at[1], device_id=(partner, tp), device_id_type=MESH)
    x_copy.start()
    pump(down_y)
    x_copy.wait_recv()
    for h in range(heads):
        mine = states[h]
        theirs = x_part[h].astype(F32)
        before = jnp.where(p == 0, mine, theirs)
        after = jnp.where(p == 0, theirs, mine)
        after_s = jnp.concatenate([after[:, :HEAD], jnp.zeros((HEAD, HEAD), F32)], axis=1)
        p_send[h] = (dot3(after[:, HEAD:], before) + after_s).astype(BF16)

    def p_copy(k, to, at):
        return pltpu.make_async_remote_copy(
            p_send, p_recv.at[at], p_ssem.at[k], p_rsem.at[k],
            device_id=(to, tp), device_id_type=MESH)

    for k in range(1, ring):
        @pl.when(r + k < ring)
        def _():
            p_copy(k, sp_of(k, 0), r).start()
    pump(early)
    for k in range(1, ring):
        @pl.when(r - k >= 0)
        def _():
            p_copy(k, sp_of(-k, 0), r - k).wait_recv()
    s_in[...] = jnp.zeros_like(s_in)

    def fold(i, _):
        for h in range(heads):
            got = p_recv[i, h].astype(F32)
            s_in[h] = dot3(got[:, HEAD:], s_in[h]) + got[:, :HEAD]
        return 0

    lax.fori_loop(0, r, fold, 0)
    for h in range(heads):
        lanes = slice(h * HEAD, (h + 1) * HEAD)
        got = x_part[h].astype(F32)
        s = s_in[h]
        s = jnp.where(p == 0, s, dot3(got[:, HEAD:], s) + got[:, :HEAD])
        att = out_scr[h, :, :HEAD] + dot3(out_scr[h, :, HEAD:], s)
        att = att * lax.rsqrt(jnp.mean(att * att, axis=-1, keepdims=True) + EPSILON) * head_gain[...]
        mixed[:, lanes] = (att * silu(gp[:, lanes].astype(F32))).astype(BF16)

    def rows_of(t):
        return pl.ds(pl.multiple_of(t * own_rows, own_rows), own_rows)

    order = [o for o in (2, 3, 1) if o < tps] + list(range(4, tps))
    d_copies = []
    for o in order:
        to = tp_peer(o)
        d_send[o - 1] = dot1(mixed[rows_of(to), :], w_out[...]).astype(BF16)
        copy = pltpu.make_async_remote_copy(
            d_send.at[o - 1], d_recv.at[o - 1], d_ssem.at[o - 1], d_rsem.at[o - 1],
            device_id=(sp, to), device_id_type=MESH)
        copy.start()
        d_copies.append(copy)
    pump(middle)
    total = dot1(mixed[rows_of(tp), :], w_out[...]).astype(BF16).astype(F32)
    for copy in d_copies:
        copy.wait_recv()
    for o in range(1, tps):
        total = total + d_recv[o - 1].astype(F32)
    total = stream[...].astype(F32) + total
    residual[...] = total
    rows_all[rows_of(tp), :] = (
        total * lax.rsqrt(jnp.mean(total * total, axis=-1, keepdims=True) + EPSILON) * feed_gain[...]
    ).astype(BF16)
    e_copies = []
    for o in order:
        copy = pltpu.make_async_remote_copy(
            rows_all.at[rows_of(tp), :], rows_all.at[rows_of(tp), :], e_ssem.at[o - 1], e_rsem.at[o - 1],
            device_id=(sp, tp_peer(o)), device_id_type=MESH)
        copy.start()
        e_copies.append(copy)
    for o in order:
        there = rows_all.at[rows_of(lax.rem(tp - o + tps, tps)), :]
        pltpu.make_async_remote_copy(
            there, there, e_ssem.at[o - 1], e_rsem.at[o - 1],
            device_id=(sp, tp_peer(o)), device_id_type=MESH).wait_recv()
    pump(later)
    need_all("G")
    need_all("U")
    for local in locals_:
        local.wait()

    tile = 128

    def ffn_in(i, _):
        lanes = pl.ds(pl.multiple_of(i * tile, tile), tile)
        both = dot1(rows_all[...], jnp.concatenate([gate_all[:, lanes], up_all[:, lanes]], axis=1))
        hidden[:, lanes] = (silu(both[:, :tile]) * both[:, tile:]).astype(BF16)
        return 0

    lax.fori_loop(0, gate_all.shape[1] // tile, ffn_in, 0)
    pump(last_group)
    need_all("D")
    dc = down_all.shape[2]
    pack = max(1, 128 // dc)
    wide = pack * dc

    def ffn_out(i, _):
        lanes = pl.ds(pl.multiple_of(i * wide, wide), wide)
        if pack == 1:
            weights = down_all[i]
        else:
            weights = jnp.concatenate([down_all[i * pack + j] for j in range(pack)], axis=1)
        f_part[:, lanes] = dot1(hidden[...], weights).astype(BF16)
        return 0

    lax.fori_loop(0, n // pack, ffn_out, 0)
    f_copies = []
    for o in order:
        copy = pltpu.make_async_remote_copy(
            f_part.at[rows_of(tp_peer(o)), :], f_recv.at[o - 1], f_ssem.at[o - 1], f_rsem.at[o - 1],
            device_id=(sp, tp_peer(o)), device_id_type=MESH)
        copy.start()
        f_copies.append(copy)
    ffn = f_part[rows_of(tp), :].astype(F32)
    for copy in f_copies:
        copy.wait_recv()
    for o in range(1, tps):
        ffn = ffn + f_recv[o - 1].astype(F32)
    result[...] = (residual[...] + ffn).astype(BF16)

    for message in copies:
        @pl.when(goes(message))
        def _():
            outgoing(message).wait_send()
    for copy in [x_copy] + d_copies + e_copies + f_copies:
        copy.wait_send()
    for k in range(1, ring):
        @pl.when(r + k < ring)
        def _():
            p_copy(k, sp_of(k, 0), r).wait_send()


def body(n, tps, stream, qp, kp, vp, gp, strength, decay_pre, extra, rate, head_gain, w_out,
         feed_gain, gate_m, up_m, down_m):
    heads, tokens = strength.shape
    own, width = stream.shape
    kr, units = gate_m.shape
    ring = n // 2
    groups = messages(ring)
    count = sum(len(g) for g in groups)
    dma = pltpu.SemaphoreType.DMA
    vmem = pl.BlockSpec(memory_space=pltpu.VMEM)
    hbm = pl.BlockSpec(memory_space=pl.ANY)
    peers = max(1, tps - 1)
    return pl.pallas_call(
        functools.partial(kernel, n, tps, groups),
        out_shape=jax.ShapeDtypeStruct((own, width), BF16),
        in_specs=[vmem] * 12 + [hbm] * 3,
        out_specs=vmem,
        scratch_shapes=[
            pltpu.VMEM((kr * n, units), BF16),
            pltpu.VMEM((kr * n, units), BF16),
            pltpu.VMEM((n,) + down_m.shape, BF16),
            pltpu.VMEM((heads, tokens, 2 * HEAD), F32),
            pltpu.VMEM((heads, HEAD, 2 * HEAD), BF16),
            pltpu.VMEM((heads, HEAD, 2 * HEAD), BF16),
            pltpu.VMEM((heads, HEAD, 2 * HEAD), BF16),
            pltpu.VMEM((ring, heads, HEAD, 2 * HEAD), BF16),
            pltpu.VMEM((heads, HEAD, HEAD), F32),
            pltpu.VMEM((tokens, heads * HEAD), BF16),
            pltpu.VMEM((peers, own, width), BF16),
            pltpu.VMEM((peers, own, width), BF16),
            pltpu.VMEM((own, width), F32),
            pltpu.VMEM((tokens, width), BF16),
            pltpu.VMEM((tokens, units), BF16),
            pltpu.VMEM((tokens, width), BF16),
            pltpu.VMEM((peers, own, width), BF16),
            dma((count,)), dma((count,)), dma((3,)), dma((2,)), dma((ring,)), dma((ring,)),
            dma((peers,)), dma((peers,)), dma((peers,)), dma((peers,)), dma((peers,)), dma((peers,)),
        ],
        compiler_params=pltpu.CompilerParams(
            collective_id=0, has_side_effects=True, vmem_limit_bytes=60 * 1024 * 1024),
    )(stream, qp, kp, vp, gp, strength, decay_pre, extra, rate[:, None], head_gain[None, :], w_out,
      feed_gain[None, :], gate_m, up_m, down_m)


def solution(mesh):
    placed = (
        P(("sp", "tp"), None),
        P("sp", "tp"),
        P("sp", "tp"),
        P("sp", "tp"),
        P("sp", "tp"),
        P("tp", "sp"),
        P("tp", "sp"),
        P("tp", "sp"),
        P("tp"),
        P(),
        P("tp", None),
        P(),
        P("sp", "tp"),
        P("sp", "tp"),
        P("tp", "sp"),
    )
    return jax.shard_map(
        functools.partial(body, mesh.shape["sp"], mesh.shape["tp"]),
        mesh=mesh, in_specs=placed, out_specs=P(("sp", "tp"), None), check_vma=False,
    )
```
